32 devices in a mesh: fs: 8 (over z, x), tp: 4 (over y, core).
Axes of the slice: x: 2, y: 2, z: 4, core: 2. Of those that a mesh axis runs over, the one named last changes fastest.
Arguments:
- tokens: bfloat16 [3584, 2304], P('fs'), may hold values from -6 to 6
- norm_gain: float32 [2304], replicated, may hold values from 0.1 to 1.9
- gate_weight: bfloat16 [2304, 6144], P('fs', 'tp'), may hold values from -0.125 to 0.125
- up_weight: bfloat16 [2304, 6144], P('fs', 'tp'), may hold values from -0.125 to 0.125
- down_weight: bfloat16 [6144, 2304], P('tp', 'fs'), may hold values from -0.078125 to 0.078125
- branch_gain: float32 [2304], replicated, may hold values from 0.1 to 1.9
Outputs:
- result: bfloat16 [3584, 2304], P('fs')
The draws below stay inside these ranges and needn't reach their ends.
All inputs are finite; a program needn't handle non-finite values.
Results may differ from the reference program's by a relative error of at most 0.014.
Values may be sent and summed in bfloat16 or wider, within the bound.
A program may use at most 64 MiB of HBM per device.

```python
import jax
import jax.numpy as jnp
from jax import lax

D = 2304
FF = 6144
TOKENS = 3584
N_TP = 4


def shard_levels(own_key, dims, split, smallest, high):
    level, own = 1.0, jax.random.fold_in(own_key, 6)
    for position, blocks in split:
        draws = jnp.exp(jax.random.uniform(jax.random.fold_in(own, position), (blocks,), jnp.float32, smallest / len(split), high / len(split)))
        level = level * jnp.repeat(draws, dims[position] // blocks).reshape([-1 if axis == position else 1 for axis in range(len(dims))])
    return level


def scatter_about(rng, shape, spread, bound, split=(), held_as=jnp.bfloat16):
    entries = jax.random.normal(rng, shape, jnp.float32) * spread
    if len(split) > 0:
        entries = shard_levels(rng, shape, split, -0.22, 0.18) * entries
    return jnp.clip(entries, min=-bound, max=bound).astype(held_as)


def setup_inputs(seed: int = 0) -> dict:
    key_of = jax.random.split(jax.random.key(seed), 7)
    tokens = scatter_about(key_of[0], (TOKENS, D), 1.0, 6.0, ((0, 8),))
    norm_gain = jnp.clip(1.0 + 0.18 * jax.random.normal(key_of[1], (D,), jnp.float32), 0.1, 1.9)
    gate_weight = scatter_about(key_of[2], (D, FF), D ** -0.5, 0.125, ((0, 8), (1, 4)))
    up_weight = scatter_about(key_of[3], (D, FF), D ** -0.5, 0.125, ((0, 8), (1, 4)))
    down_weight = scatter_about(key_of[4], (FF, D), FF ** -0.5, 0.078125, ((0, 4), (1, 8)))
    branch_gain = jnp.clip(1.0 + 0.18 * jax.random.normal(key_of[5], (D,), jnp.float32), 0.1, 1.9)
    return {"tokens": tokens, "norm_gain": norm_gain, "gate_weight": gate_weight, "up_weight": up_weight, "down_weight": down_weight, "branch_gain": branch_gain}


epsilon = 1e-06

def reference(tokens, norm_gain, gate_weight, up_weight, down_weight, branch_gain):
    widened = tokens.astype(jnp.float32)
    scale = lax.rsqrt(lax.optimization_barrier(jnp.mean(widened * widened, axis=-1, keepdims=True)) + epsilon)
    normed = (widened * scale * norm_gain).astype(jnp.bfloat16)
    width = FF // N_TP
    branch = jnp.zeros(tokens.shape, jnp.float32)
    for block_index in range(N_TP):
        begin = block_index * width
        gate_sum = jnp.dot(normed, gate_weight[:, begin:begin + width], preferred_element_type=jnp.float32)
        up_sum = jnp.dot(normed, up_weight[:, begin:begin + width], preferred_element_type=jnp.float32)
        hidden = (jax.nn.silu(gate_sum) * up_sum).astype(jnp.bfloat16)
        partial_value = jnp.dot(hidden, down_weight[begin:begin + width, :], preferred_element_type=jnp.float32)
        branch = branch + partial_value.astype(jnp.bfloat16).astype(jnp.float32)
    branch_scale = lax.rsqrt(lax.optimization_barrier(jnp.mean(branch * branch, axis=-1, keepdims=True)) + epsilon)
    return (widened + branch * branch_scale * branch_gain).astype(jnp.bfloat16)
```

```python
import functools

import jax
import jax.numpy as jnp
from jax import lax
from jax.experimental import pallas as pl
from jax.experimental.pallas import tpu as pltpu
from jax.sharding import PartitionSpec as P

MESH = pl.DeviceIdType.MESH
epsilon = 1e-06
GATE, UP, DOWN = 0, 1, 2
SUB = 3
STRIP = 16


def complete(own_tokens, summed, branch_gain):
    branch_scale = lax.rsqrt(jnp.mean(summed * summed, axis=-1, keepdims=True) + epsilon)
    return (own_tokens.astype(jnp.float32) + summed * branch_scale * branch_gain).astype(
        jnp.bfloat16
    )


def normalize(tokens, norm_gain):
    widened = tokens.astype(jnp.float32)
    scale = lax.rsqrt(jnp.mean(widened * widened, axis=-1, keepdims=True) + epsilon)
    return (widened * scale * norm_gain).astype(jnp.bfloat16)


def plain(tokens, norm_gain, gate_weight, up_weight, down_weight, branch_gain):
    normed = normalize(tokens, norm_gain)
    gate_whole, up_whole = (
        lax.all_gather(gate_weight, "fs", axis=0, tiled=True),
        lax.all_gather(up_weight, "fs", axis=0, tiled=True),
    )
    gate_sum = jnp.dot(normed, gate_whole, preferred_element_type=jnp.float32)
    up_sum = jnp.dot(normed, up_whole, preferred_element_type=jnp.float32)
    hidden = (jax.nn.silu(gate_sum) * up_sum).astype(jnp.bfloat16)
    partial_value = jnp.dot(
        hidden,
        lax.all_gather(down_weight, "fs", axis=1, tiled=True),
        preferred_element_type=jnp.float32,
    )
    summed = lax.psum(partial_value.astype(jnp.bfloat16), "tp").astype(jnp.float32)
    return complete(tokens, summed, branch_gain)


def kernel(tokens_ref, gate_ref, up_ref, down_ref, gain_ref, out_ref, *scratch):
    xs, xn, wg, wu, wd, gated, hid, part, pc, sm, r_end, r_mid, r_fin = scratch[:13]
    (loc_sem, z_send, z_recv, x_send, x_recv, y_send, y_recv, dx_send, dx_recv, dy_send, dy_recv,
     t_send, t_recv, td_send, td_recv, c_send, c_recv, e_send, e_recv, m_send, m_recv, f_send, f_recv,
     o_send, o_recv) = scratch[13:]
    f, t = lax.axis_index("fs"), lax.axis_index("tp")
    z, x, y, c = f // 2, f % 2, t // 2, t % 2
    h = z // 2
    middling = (z % 2 + z // 2) % 2
    is_mid, is_end = middling == 1, middling == 0
    plane = [z, z + 1 - 2 * (z % 2), 2 - h, 3 - 3 * h]
    slot = [0, 1, 3 - middling, 3 - middling]
    depth, width = gate_ref.shape[0], wg.shape[1] // 2
    rq, d = xn.shape[2:]
    strips = rq // STRIP
    chunks, cw = part.shape[0], part.shape[-1]
    rows = 8 * rq
    weights, inputs = (wg, wu, wd), (gate_ref, up_ref, down_ref)

    x_to, y_to, c_to = (f + 1 - 2 * x, t), (f, (t + 2) % 4), (f, t + 1 - 2 * c)
    yc_to = (f, (1 - y) * 2 + 1 - c)

    def z_to(k):
        return (plane[k] * 2 + x, t)

    barrier = pltpu.get_barrier_semaphore()
    for peer in (x_to, y_to, c_to, yc_to, z_to(1), z_to(2), z_to(3)):
        pl.semaphore_signal(barrier, inc=1, device_id=peer, device_id_type=MESH)

    def remote(src, dst, send, recv, to):
        return pltpu.make_async_remote_copy(
            src, dst, send, recv, device_id=to, device_id_type=MESH
        )

    def block(a, k, yy, lo=0, n=depth, flip=0):
        ff = plane[k] * 2 + (1 - x if flip else x)
        at = pl.ds(pl.multiple_of(ff * depth + lo, STRIP), n)
        return weights[a].at[at, pl.ds(pl.multiple_of(yy * width, width), width)]

    def quarter(a, k):
        return inputs[a].at[:, pl.ds(pl.multiple_of(plane[k] * width, width), width)]

    local = [pltpu.make_async_copy(tokens_ref.at[t], xs, loc_sem.at[3])] + [
        pltpu.make_async_copy(quarter(a, 0), block(a, 0, y), loc_sem.at[a]) for a in range(3)
    ]
    for copy in local:
        copy.start()

    sent = []
    sent_end, sent_mid = [], []

    def start(copy):
        copy.start()
        sent.append(copy)

    def start_end(copy):
        pl.when(is_end)(copy.start)
        sent_end.append(copy)

    def start_mid(copy):
        pl.when(is_mid)(copy.start)
        sent_mid.append(copy)

    def z_copy(a, k):
        return remote(
            quarter(a, k), block(a, 0, y), z_send.at[a, k], z_recv.at[a, slot[k]], z_to(k)
        )

    def z_wait(a, k):
        piece = block(a, k, y)
        remote(piece, piece, z_send.at[a, k], z_recv.at[a, k], z_to(k)).wait_recv()

    def across(a, k):
        src = quarter(a, 0) if k == 0 else block(a, k, y)
        return (
            remote(src, block(a, k, y), x_send.at[a, k], x_recv.at[a, k], x_to),
            remote(src, block(a, k, y), y_send.at[a, k], y_recv.at[a, k], y_to),
        )

    def diagonal(a, k):
        n = depth // 2
        first, second = block(a, k, y, 0, n, 1), block(a, k, 1 - y, n, n)
        return (
            remote(first, first, dy_send.at[a, k], dy_recv.at[a, k], y_to),
            remote(second, second, dx_send.at[a, k], dx_recv.at[a, k], x_to),
        )

    def spread(a, k):
        if k > 0:
            z_wait(a, k)
        for copy in across(a, k):
            start(copy)

    def relay(a, k):
        for got, on in zip(across(a, k), diagonal(a, k)):
            got.wait_recv()
            start(on)

    def settle(a, k):
        for got in diagonal(a, k):
            got.wait_recv()

    def strip(k, s):
        return xn.at[plane[k], c, pl.ds(s * STRIP, STRIP)]

    def token_copy(lane, k, s, to, slot):
        piece = strip(k, s)
        return remote(piece, piece, t_send.at[lane, s], t_recv.at[slot, s], to)

    def token_wait(k, s):
        token_copy(0, k, s, z_to(1), k).wait_recv()

    def token_pair(k):
        piece = xn.at[plane[k], c]
        return remote(piece, piece, td_send.at[k], td_recv.at[k], c_to)

    def token_relay(k, lane, to, slot, lo=0, hi=strips):
        for s in range(lo, hi):
            pl.when(is_mid)(lambda s=s: token_wait(k, s))
            start_mid(token_copy(lane, k, s, z_to(to), slot))
        if hi == strips:
            start_mid(token_pair(k))

    def token_take(k):
        for s in range(strips):
            pl.when(is_end)(lambda s=s: token_wait(k, s))
        start_end(token_pair(k))

    def from_near():
        token_relay(1, 2, 2, 3)

    def from_mid(lo=0, hi=strips):
        token_relay(2, 3, 1, 2, lo, hi)

    def from_far(lo=0, hi=strips):
        token_relay(3, 4, 1, 3, lo, hi)

    def token_settle(*which):
        for k in which:
            token_pair(k).wait_recv()

    pl.semaphore_wait(barrier, 7)

    def sends(role, pairs):
        for a, k in pairs:
            role(z_copy(a, k))

    sends(start_end, [(GATE, 1), (GATE, 2), (GATE, 3), (UP, 1), (UP, 2), (UP, 3)])
    sends(start_mid, [(GATE, 2), (GATE, 1), (GATE, 3), (UP, 2), (UP, 1), (UP, 3)])
    spread(GATE, 0)
    spread(UP, 0)

    local[0].wait()
    for s in range(strips):
        at_rows = pl.ds(s * STRIP, STRIP)
        v = xs[at_rows, :].astype(jnp.float32)
        scale = lax.rsqrt(jnp.mean(v * v, axis=-1, keepdims=True) + epsilon)
        xn[z, c, at_rows, :] = (v * scale * gain_ref[...]).astype(jnp.bfloat16)
    for s in range(strips):
        start(token_copy(0, 0, s, z_to(1), 1))
        start_mid(token_copy(1, 0, s, z_to(2), 2))
    start(token_pair(0))
    sends(start_end, [(DOWN, 1)])

    def product(w, zb, nb, n0, nw):
        v = xn[pl.ds(zb, nb)].reshape(nb * 2 * rq, d)
        return jnp.dot(
            v, w[:, pl.ds(pl.multiple_of(n0, nw), nw)], preferred_element_type=jnp.float32
        )

    def gate_rows(zb, nb):
        def one(i, carry):
            n0 = pl.multiple_of(i * width, width)
            v = product(wg, zb, nb, n0, width)
            v = v / (1.0 + jnp.exp(-v))
            gated[pl.ds(zb, nb), :, pl.ds(n0, width)] = v.reshape(nb, 2 * rq, width)
            return carry

        lax.fori_loop(0, 2, one, 0)

    def up_rows(zb, nb):
        def one(i, carry):
            n0 = pl.multiple_of(i * width, width)
            v = product(wu, zb, nb, n0, width).reshape(nb, 2 * rq, width)
            v = gated[pl.ds(zb, nb), :, pl.ds(n0, width)] * v
            hid[pl.ds(zb, nb), :, pl.ds(n0, width)] = v.astype(jnp.bfloat16)
            return carry

        lax.fori_loop(0, 2, one, 0)

    relay(GATE, 0)
    spread(GATE, 1)
    relay(UP, 0)
    spread(GATE, 2)
    relay(GATE, 1)
    spread(GATE, 3)
    spread(UP, 1)
    relay(GATE, 2)
    spread(UP, 2)
    relay(GATE, 3)
    relay(UP, 1)
    spread(UP, 3)
    spread(DOWN, 0)
    from_near()
    sends(start_mid, [(DOWN, 2), (DOWN, 3)])
    from_mid(0, 4)
    relay(UP, 2)
    for copy in local[1:]:
        copy.wait()
    for k in range(4):
        settle(GATE, k)
    token_take(1)
    token_settle(0, 1)
    gate_rows(h * 2, 2)
    from_mid(4)
    sends(start_mid, [(DOWN, 1)])
    relay(UP, 3)
    from_far(0, 4)
    token_take(2)
    token_settle(2)
    gate_rows(plane[2], 1)
    from_far(4)
    sends(start_end, [(DOWN, 2), (DOWN, 3)])
    spread(DOWN, 1)
    for k in range(4):
        settle(UP, k)
    up_rows(h * 2, 2)
    up_rows(plane[2], 1)
    relay(DOWN, 0)
    relay(DOWN, 1)
    token_take(3)
    token_settle(3)
    gate_rows(plane[3], 1)
    up_rows(plane[3], 1)

    def column(i):
        first = SUB - 1 - i if i < SUB else i
        return h * (chunks - 1) + (1 - 2 * h) * first

    def pair_copy(i):
        j = column(i)
        return remote(part.at[j, :, 1 - c], pc.at[j], c_send.at[j], c_recv.at[j], c_to)

    def down_chunk(i):
        j = column(i)
        value = lax.dot_general(
            hid[...].reshape(rows, 2 * width), wd[pl.ds(pl.multiple_of(j * cw, cw), cw), :], (((1,), (1,)), ((), ())),
            preferred_element_type=jnp.float32,
        ).astype(jnp.bfloat16)
        for zz in range(4):
            for cc in range(2):
                at = (zz * 2 + cc) * rq
                part[j, zz, cc] = value[at:at + rq]
        start(pair_copy(i))

    def add(*terms):
        return functools.reduce(lambda a, b: a + b, [v.astype(jnp.float32) for v in terms])

    def end_copies(i):
        j = column(i)
        return (
            remote(sm.at[j, pl.ds(2, 2)], r_end.at[j, pl.ds(1, 2)], e_send.at[j, 0], e_recv.at[j, 0], z_to(1)),
            remote(sm.at[j, 1], r_end.at[j, 0], e_send.at[j, 1], e_recv.at[j, 1], z_to(1)),
        )

    def mid_copy(i):
        j = column(i)
        return remote(sm.at[j, pl.ds(2, 2)], r_mid.at[j], m_send.at[j], m_recv.at[j], z_to(2))

    def fin_copy(i):
        j = column(i)
        return remote(sm.at[j, 1], r_fin.at[j], f_send.at[j], f_recv.at[j], z_to(1))

    def pair_sum(i):
        pair_copy(i).wait_recv()
        j = column(i)
        for k in range(4):
            sm[j, k] = add(part[j, plane[k], c], pc[j, plane[k]]).astype(jnp.bfloat16)
        start_end(end_copies(i)[0])

    def end_rest(*which):
        for i in which:
            start_end(end_copies(i)[1])

    def pass_on(i):
        j = column(i)
        end_copies(i)[0].wait_recv()
        sm[j, 2] = add(sm[j, 2], r_end[j, 1]).astype(jnp.bfloat16)
        sm[j, 3] = add(sm[j, 3], r_end[j, 2]).astype(jnp.bfloat16)
        mid_copy(i).start()

    def pass_early(i):
        pl.when(is_mid)(lambda: pass_on(i))

    def piece(i, tt):
        return out_ref.at[tt, :, pl.ds(pl.multiple_of(column(i) * cw, cw), cw)]

    def share_copies(i):
        j, own, other = column(i), piece(i, t), piece(i, (t + 2) % 4)
        return [
            remote(src, src, o_send.at[j, n], o_recv.at[j, n], to)
            for n, (src, to) in enumerate(((own, y_to), (own, c_to), (other, c_to)))
        ]

    def share(i):
        for copy in share_copies(i)[:2]:
            copy.start()

    def hand_back(i):
        j = column(i)
        mid_copy(i).wait_recv()
        sm[j, 1] = add(sm[j, 1], r_mid[j, 1]).astype(jnp.bfloat16)
        fin_copy(i).start()

    def finish_mid(i):
        j = column(i)
        at = pl.ds(pl.multiple_of(j * cw, cw), cw)
        end_copies(i)[1].wait_recv()
        out_ref[t, :, at] = add(sm[j, 0], r_end[j, 0], r_mid[j, 0]).astype(jnp.bfloat16)
        share(i)

    def finish_end(i):
        j = column(i)
        at = pl.ds(pl.multiple_of(j * cw, cw), cw)
        fin_copy(i).wait_recv()
        out_ref[t, :, at] = add(sm[j, 0], r_fin[j]).astype(jnp.bfloat16)
        share(i)

    def forward(i):
        copies = share_copies(i)
        copies[0].wait_recv()
        copies[2].start()

    spread(DOWN, 2)
    settle(DOWN, 0)
    settle(DOWN, 1)
    down_chunk(0)
    down_chunk(1)
    pair_sum(0)
    down_chunk(2)
    pair_sum(1)
    pair_sum(2)
    end_rest(0, 1, 2)
    relay(DOWN, 2)
    pass_early(0)
    spread(DOWN, 3)
    pass_early(1)
    settle(DOWN, 2)
    down_chunk(3)
    pair_sum(3)
    relay(DOWN, 3)
    pass_early(2)
    settle(DOWN, 3)
    down_chunk(4)
    down_chunk(5)
    pair_sum(4)
    pair_sum(5)
    end_rest(3, 4, 5)

    @pl.when(is_mid)
    def _():
        hand_back(3)
        pass_on(3)
        hand_back(4)
        hand_back(5)
        pass_on(4)
        hand_back(0)
        pass_on(5)
        finish_mid(0)
        hand_back(1)
        finish_mid(1)
        forward(0)
        finish_mid(3)
        forward(1)
        hand_back(2)
        finish_mid(2)
        finish_mid(4)
        forward(3)
        forward(2)
        finish_mid(5)
        forward(4)
        forward(5)

    @pl.when(is_end)
    def _():
        finish_end(3)
        finish_end(4)
        forward(3)
        finish_end(5)
        forward(4)
        finish_end(0)
        forward(5)
        finish_end(1)
        forward(0)
        finish_end(2)
        forward(1)
        forward(2)

    for i in range(chunks):
        for copy in share_copies(i)[1:]:
            copy.wait_recv()
        for copy in share_copies(i):
            copy.wait_send()

    for copy in sent:
        copy.wait_send()

    @pl.when(is_end)
    def _():
        for copy in sent_end:
            copy.wait_send()

    @pl.when(is_mid)
    def _():
        for copy in sent_mid:
            copy.wait_send()
        for i in range(chunks):
            mid_copy(i).wait_send()
            fin_copy(i).wait_send()


def fused(tokens, norm_gain, gate_weight, up_weight, down_weight, branch_gain):
    rows, d = tokens.shape
    n_tp, planes = 4, 4
    rq = rows // n_tp
    hidden = gate_weight.shape[1]
    width = 2 * (hidden // planes)
    chunks = 2 * SUB
    cw = d // chunks
    bf16, f32, dma = jnp.bfloat16, jnp.float32, pltpu.SemaphoreType.DMA
    hbm = pl.BlockSpec(memory_space=pl.ANY)
    vmem = pl.BlockSpec(memory_space=pltpu.VMEM)
    out = pl.pallas_call(
        kernel,
        out_shape=jax.ShapeDtypeStruct((n_tp, rq, d), bf16),
        in_specs=[hbm] * 4 + [vmem],
        out_specs=vmem,
        scratch_shapes=[
            pltpu.VMEM((rq, d), bf16),
            pltpu.VMEM((planes, 2, rq, d), bf16),
            pltpu.VMEM((d, width), bf16),
            pltpu.VMEM((d, width), bf16),
            pltpu.VMEM((d, width), bf16),
            pltpu.VMEM((planes, 2 * rq, width), f32),
            pltpu.VMEM((planes, 2 * rq, width), bf16),
            pltpu.VMEM((chunks, planes, 2, rq, cw), bf16),
            pltpu.VMEM((chunks, planes, rq, cw), bf16),
            pltpu.VMEM((chunks, planes, rq, cw), bf16),
            pltpu.VMEM((chunks, 3, rq, cw), bf16),
            pltpu.VMEM((chunks, 2, rq, cw), bf16),
            pltpu.VMEM((chunks, rq, cw), bf16),
            dma((4,)),
            dma((3, 4)), dma((3, 4)),
            dma((3, 4)), dma((3, 4)),
            dma((3, 4)), dma((3, 4)),
            dma((3, 4)), dma((3, 4)),
            dma((3, 4)), dma((3, 4)),
            dma((5, rq // STRIP)), dma((4, rq // STRIP)),
            dma((4,)), dma((4,)),
            dma((chunks,)), dma((chunks,)),
            dma((chunks, 2)), dma((chunks, 2)),
            dma((chunks,)), dma((chunks,)),
            dma((chunks,)), dma((chunks,)),
            dma((chunks, 3)), dma((chunks, 3)),
        ],
        compiler_params=pltpu.CompilerParams(
            collective_id=0, has_side_effects=True, vmem_limit_bytes=60 * 1024 * 1024
        ),
    )(
        tokens.reshape(n_tp, rq, d), gate_weight, up_weight, down_weight.T, norm_gain.reshape(1, d),
    )
    return complete(tokens, out.reshape(rows, d).astype(jnp.float32), branch_gain)


def solution(mesh):
    n_fs, n_tp = mesh.shape["fs"], mesh.shape["tp"]

    def per_device(*args):
        tokens, _, gate_weight = args[:3]
        rows, d = tokens.shape
        depth, hidden = gate_weight.shape
        fits = (
            n_fs == 8
            and n_tp == 4
            and rows % (STRIP * n_tp) == 0
            and depth % (2 * STRIP) == 0
            and hidden % (128 * 4) == 0
            and d % (128 * 2 * SUB) == 0
        )
        if fits:
            return fused(*args)
        return plain(*args)

    in_specs = (P("fs", None), P(), P("fs", "tp"), P("fs", "tp"), P("tp", "fs"), P())
    return jax.shard_map(
        per_device, mesh=mesh, in_specs=in_specs, out_specs=P("fs", None), check_vma=False
    )
```

```python
import functools

import jax
import jax.numpy as jnp
from jax import lax
from jax.experimental import pallas as pl
from jax.experimental.pallas import tpu as pltpu
from jax.sharding import PartitionSpec as P

MESH = pl.DeviceIdType.MESH
epsilon = 1e-06
GATE, UP, DOWN = 0, 1, 2
SUB = 3
STRIP = 16


def complete(own_tokens, summed, branch_gain):
    branch_scale = lax.rsqrt(jnp.mean(summed * summed, axis=-1, keepdims=True) + epsilon)
    return (own_tokens.astype(jnp.float32) + summed * branch_scale * branch_gain).astype(
        jnp.bfloat16
    )


def normalize(tokens, norm_gain):
    widened = tokens.astype(jnp.float32)
    scale = lax.rsqrt(jnp.mean(widened * widened, axis=-1, keepdims=True) + epsilon)
    return (widened * scale * norm_gain).astype(jnp.bfloat16)


def plain(tokens, norm_gain, gate_weight, up_weight, down_weight, branch_gain):
    normed = normalize(tokens, norm_gain)
    gate_whole, up_whole = (
        lax.all_gather(gate_weight, "fs", axis=0, tiled=True),
        lax.all_gather(up_weight, "fs", axis=0, tiled=True),
    )
    gate_sum = jnp.dot(normed, gate_whole, preferred_element_type=jnp.float32)
    up_sum = jnp.dot(normed, up_whole, preferred_element_type=jnp.float32)
    hidden = (jax.nn.silu(gate_sum) * up_sum).astype(jnp.bfloat16)
    partial_value = jnp.dot(
        hidden,
        lax.all_gather(down_weight, "fs", axis=1, tiled=True),
        preferred_element_type=jnp.float32,
    )
    summed = lax.psum(partial_value.astype(jnp.bfloat16), "tp").astype(jnp.float32)
    return complete(tokens, summed, branch_gain)


def kernel(tokens_ref, gate_ref, up_ref, down_ref, norm_gain_ref, branch_gain_ref, result_ref, *scratch):
    xs, gains, out_ref, xn, wg, wu, wd, gated, hid, part, pc, sm, r_end, r_mid, r_fin = scratch[:15]
    (loc_sem, z_send, z_recv, x_send, x_recv, y_send, y_recv, dx_send, dx_recv, dy_send, dy_recv,
     t_send, t_recv, td_send, td_recv, c_send, c_recv, e_send, e_recv, m_send, m_recv, f_send, f_recv,
     o_send, o_recv, w_sem) = scratch[15:]
    f, t = lax.axis_index("fs"), lax.axis_index("tp")
    z, x, y, c = f // 2, f % 2, t // 2, t % 2
    h = z // 2
    middling = (z % 2 + z // 2) % 2
    is_mid, is_end = middling == 1, middling == 0
    plane = [z, z + 1 - 2 * (z % 2), 2 - h, 3 - 3 * h]
    slot = [0, 1, 3 - middling, 3 - middling]
    depth, width = gate_ref.shape[0], wg.shape[1] // 2
    rq, d = xn.shape[2:]
    strips = rq // STRIP
    chunks, cw = part.shape[0], part.shape[-1]
    rows = 8 * rq
    weights, inputs = (wg, wu, wd), (gate_ref, up_ref, down_ref)

    x_to, y_to, c_to = (f + 1 - 2 * x, t), (f, (t + 2) % 4), (f, t + 1 - 2 * c)
    yc_to = (f, (1 - y) * 2 + 1 - c)

    def z_to(k):
        return (plane[k] * 2 + x, t)

    barrier = pltpu.get_barrier_semaphore()
    for peer in (x_to, y_to, c_to, yc_to, z_to(1), z_to(2), z_to(3)):
        pl.semaphore_signal(barrier, inc=1, device_id=peer, device_id_type=MESH)

    def remote(src, dst, send, recv, to):
        return pltpu.make_async_remote_copy(
            src, dst, send, recv, device_id=to, device_id_type=MESH
        )

    def block(a, k, yy, lo=0, n=depth, flip=0):
        ff = plane[k] * 2 + (1 - x if flip else x)
        at = pl.ds(pl.multiple_of(ff * depth + lo, STRIP), n)
        return weights[a].at[at, pl.ds(pl.multiple_of(yy * width, width), width)]

    def quarter(a, k):
        return inputs[a].at[:, pl.ds(pl.multiple_of(plane[k] * width, width), width)]

    early = [
        pltpu.make_async_copy(tokens_ref, xs, loc_sem.at[3]),
        pltpu.make_async_copy(norm_gain_ref, gains.at[0, 0], loc_sem.at[4]),
        pltpu.make_async_copy(branch_gain_ref, gains.at[1, 0], loc_sem.at[5]),
    ]
    local = early + [
        pltpu.make_async_copy(quarter(a, 0), block(a, 0, y), loc_sem.at[a]) for a in range(3)
    ]
    for copy in local:
        copy.start()

    def z_copy(a, k):
        return remote(
            quarter(a, k), block(a, 0, y), z_send.at[a, k], z_recv.at[a, slot[k]], z_to(k)
        )

    def z_wait(a, k):
        piece = block(a, k, y)
        remote(piece, piece, z_send.at[a, k], z_recv.at[a, k], z_to(k)).wait_recv()

    def across(a, k):
        src = quarter(a, 0) if k == 0 else block(a, k, y)
        return (
            remote(src, block(a, k, y), x_send.at[a, k], x_recv.at[a, k], x_to),
            remote(src, block(a, k, y), y_send.at[a, k], y_recv.at[a, k], y_to),
        )

    def diagonal(a, k):
        n = depth // 2
        first, second = block(a, k, y, 0, n, 1), block(a, k, 1 - y, n, n)
        return (
            remote(first, first, dy_send.at[a, k], dy_recv.at[a, k], y_to),
            remote(second, second, dx_send.at[a, k], dx_recv.at[a, k], x_to),
        )

    def spread(a, k):
        if k > 0:
            z_wait(a, k)
        for copy in across(a, k):
            copy.start()

    def relay(a, k):
        for got, on in zip(across(a, k), diagonal(a, k)):
            got.wait_recv()
            on.start()

    def settle(a, k):
        for got in diagonal(a, k):
            got.wait_recv()

    def strip(k, s):
        return xn.at[plane[k], c, pl.ds(s * STRIP, STRIP)]

    def token_copy(lane, k, s, to, slot):
        piece = strip(k, s)
        return remote(piece, piece, t_send.at[lane, s], t_recv.at[slot, s], to)

    def token_wait(k, s):
        token_copy(0, k, s, z_to(1), k).wait_recv()

    def token_pair(k):
        piece = xn.at[plane[k], c]
        return remote(piece, piece, td_send.at[k], td_recv.at[k], c_to)

    def token_lanes(mid):
        if mid:
            return [(0, 1, 1), (0, 2, 2), (1, 2, 3), (2, 1, 2), (3, 1, 3)]
        return [(0, 1, 1)]

    def token_relay(mid, lane, lo=0, hi=strips):
        k, to, there = token_lanes(mid)[lane]
        for s in range(lo, hi):
            if k > 0:
                token_wait(k, s)
            token_copy(lane, k, s, z_to(to), there).start()
        if k > 0 and hi == strips:
            token_pair(k).start()

    def token_take(k):
        for s in range(strips):
            token_wait(k, s)
        token_pair(k).start()

    def token_settle(*which):
        for k in which:
            token_pair(k).wait_recv()

    pl.semaphore_wait(barrier, 7)

    def sends(*pairs):
        for a, k in pairs:
            z_copy(a, k).start()

    @pl.when(is_end)
    def _():
        sends((GATE, 1), (GATE, 2), (GATE, 3), (UP, 1), (UP, 2), (UP, 3))

    @pl.when(is_mid)
    def _():
        sends((GATE, 2), (GATE, 1), (GATE, 3), (UP, 2), (UP, 1), (UP, 3))

    spread(GATE, 0)
    spread(UP, 0)

    for copy in early:
        copy.wait()
    for s in range(strips):
        at_rows = pl.ds(s * STRIP, STRIP)
        v = xs[t, at_rows, :].astype(jnp.float32)
        scale = lax.rsqrt(jnp.mean(v * v, axis=-1, keepdims=True) + epsilon)
        xn[z, c, at_rows, :] = (v * scale * gains[0]).astype(jnp.bfloat16)
    token_pair(0).start()

    @pl.when(is_end)
    def _():
        token_relay(False, 0)
        sends((DOWN, 1))

    @pl.when(is_mid)
    def _():
        token_relay(True, 1)
        token_relay(True, 0)

    def product(w, zb, nb, n0, nw):
        v = xn[pl.ds(zb, nb)].reshape(nb * 2 * rq, d)
        return jnp.dot(
            v, w[:, pl.ds(pl.multiple_of(n0, nw), nw)], preferred_element_type=jnp.float32
        )

    def gate_rows(zb, nb):
        def one(i, carry):
            n0 = pl.multiple_of(i * width, width)
            v = product(wg, zb, nb, n0, width)
            v = v / (1.0 + jnp.exp(-v))
            gated[pl.ds(zb, nb), :, pl.ds(n0, width)] = v.reshape(nb, 2 * rq, width)
            return carry

        lax.fori_loop(0, 2, one, 0)

    def up_rows(zb, nb):
        def one(i, carry):
            n0 = pl.multiple_of(i * width, width)
            v = product(wu, zb, nb, n0, width).reshape(nb, 2 * rq, width)
            v = gated[pl.ds(zb, nb), :, pl.ds(n0, width)] * v
            hid[pl.ds(zb, nb), :, pl.ds(n0, width)] = v.astype(jnp.bfloat16)
            return carry

        lax.fori_loop(0, 2, one, 0)

    def settle_all(a):
        for k in range(4):
            settle(a, k)

    def own_weights():
        for copy in local[3:]:
            copy.wait()

    @pl.when(is_end)
    def _():
        relay(GATE, 0)
        spread(GATE, 1)
        relay(UP, 0)
        spread(UP, 1)
        relay(GATE, 1)
        spread(GATE, 2)
        relay(UP, 1)
        spread(GATE, 3)
        relay(GATE, 2)
        spread(UP, 2)
        relay(GATE, 3)
        spread(UP, 3)
        relay(UP, 2)
        token_take(1)
        relay(UP, 3)
        spread(DOWN, 0)
        settle_all(GATE)
        own_weights()
        token_settle(0, 1)
        gate_rows(h * 2, 2)
        settle_all(UP)
        up_rows(h * 2, 2)
        sends((DOWN, 3), (DOWN, 2))
        token_take(2)
        relay(DOWN, 0)
        token_settle(2)
        gate_rows(plane[2], 1)
        up_rows(plane[2], 1)
        spread(DOWN, 1)
        token_take(3)
        token_settle(3)
        gate_rows(plane[3], 1)
        relay(DOWN, 1)
        up_rows(plane[3], 1)
        spread(DOWN, 2)
        settle(DOWN, 0)

    @pl.when(is_mid)
    def _():
        relay(GATE, 0)
        spread(GATE, 1)
        relay(UP, 0)
        spread(GATE, 2)
        relay(GATE, 1)
        spread(GATE, 3)
        spread(UP, 1)
        relay(GATE, 2)
        spread(UP, 2)
        relay(GATE, 3)
        relay(UP, 1)
        spread(UP, 3)
        sends((DOWN, 1))
        token_relay(True, 2)
        token_relay(True, 3, 0, 3)
        relay(UP, 2)
        token_relay(True, 3, 3)
        token_relay(True, 4, 0, 4)
        relay(UP, 3)
        spread(DOWN, 0)
        settle_all(GATE)
        own_weights()
        token_settle(0, 1)
        gate_rows(h * 2, 2)
        token_relay(True, 4, 4)
        sends((DOWN, 3), (DOWN, 2))
        settle_all(UP)
        up_rows(h * 2, 2)
        relay(DOWN, 0)
        spread(DOWN, 1)
        token_settle(2)
        gate_rows(plane[2], 1)
        up_rows(plane[2], 1)
        relay(DOWN, 1)
        token_settle(3)
        gate_rows(plane[3], 1)
        up_rows(plane[3], 1)
        settle(DOWN, 0)

    def column(i):
        return h * (chunks - 1) + (1 - 2 * h) * i

    def pair_copy(i):
        j = column(i)
        return remote(part.at[j, :, 1 - c], pc.at[j], c_send.at[j], c_recv.at[j], c_to)

    def down_chunk(i):
        j = column(i)
        value = lax.dot_general(
            hid[...].reshape(rows, 2 * width), wd[pl.ds(pl.multiple_of(j * cw, cw), cw), :], (((1,), (1,)), ((), ())),
            preferred_element_type=jnp.float32,
        ).astype(jnp.bfloat16)
        for zz in range(4):
            for cc in range(2):
                at = (zz * 2 + cc) * rq
                part[j, zz, cc] = value[at:at + rq]
        pair_copy(i).start()

    def add(*terms):
        return functools.reduce(lambda a, b: a + b, [v.astype(jnp.float32) for v in terms])

    first = (rq // STRIP + 1) // 2 * STRIP
    whole, halves = [(0, rq)], [(0, first), (first, rq - first)]

    def outward(i):
        return halves if i >= chunks - 2 else whole

    def inward(i):
        return halves if i < 2 else whole

    def end_copies(i):
        j = column(i)
        return [
            remote(
                sm.at[j, pl.ds(2, 2), pl.ds(lo, n)], r_end.at[j, pl.ds(1, 2), pl.ds(lo, n)],
                e_send.at[j, p], e_recv.at[j, p], z_to(1),
            )
            for p, (lo, n) in enumerate(outward(i))
        ]

    def end_copy(i):
        j = column(i)
        return remote(sm.at[j, 1], r_end.at[j, 0], e_send.at[j, 2], e_recv.at[j, 2], z_to(1))

    def mid_copies(i, parts):
        j = column(i)
        return [
            remote(
                sm.at[j, pl.ds(2, 2), pl.ds(lo, n)], r_mid.at[j, :, pl.ds(lo, n)],
                m_send.at[j, p], m_recv.at[j, p], z_to(2),
            )
            for p, (lo, n) in enumerate(parts)
        ]

    def fin_copies(i):
        j = column(i)
        return [
            remote(
                sm.at[j, 1, pl.ds(lo, n)], r_fin.at[j, pl.ds(lo, n)],
                f_send.at[j, p], f_recv.at[j, p], z_to(1),
            )
            for p, (lo, n) in enumerate(inward(i))
        ]

    def pair_sum(i):
        pair_copy(i).wait_recv()
        j = column(i)
        for k in range(4):
            sm[j, k] = add(part[j, plane[k], c], pc[j, plane[k]]).astype(jnp.bfloat16)

        @pl.when(is_end)
        def _():
            for copy in end_copies(i):
                copy.start()

    def end_rest(*which):
        for i in which:
            end_copy(i).start()

    def pass_on(i):
        j = column(i)
        for (lo, n), got, on in zip(outward(i), end_copies(i), mid_copies(i, outward(i))):
            at = pl.ds(lo, n)
            got.wait_recv()
            sm[j, 2, at] = add(sm[j, 2, at], r_end[j, 1, at]).astype(jnp.bfloat16)
            sm[j, 3, at] = add(sm[j, 3, at], r_end[j, 2, at]).astype(jnp.bfloat16)
            on.start()

    def share_copies(i):
        j = column(i)
        lanes = pl.ds(pl.multiple_of(j * cw, cw), cw)
        every = []
        for p, (lo, n) in enumerate(inward(i)):
            own, other = out_ref.at[t, pl.ds(lo, n), lanes], out_ref.at[(t + 2) % 4, pl.ds(lo, n), lanes]
            every.append([
                remote(src, src, o_send.at[j, 3 * p + k], o_recv.at[j, 3 * p + k], to)
                for k, (src, to) in enumerate(((own, y_to), (own, c_to), (other, c_to)))
            ])
        return every

    def share(i, p):
        for copy in share_copies(i)[p][:2]:
            copy.start()

    def hand_back(i):
        j = column(i)
        for (lo, n), got, on in zip(inward(i), mid_copies(i, inward(i)), fin_copies(i)):
            at = pl.ds(lo, n)
            got.wait_recv()
            sm[j, 1, at] = add(sm[j, 1, at], r_mid[j, 1, at]).astype(jnp.bfloat16)
            on.start()

    def finish_mid(i):
        j = column(i)
        lanes = pl.ds(pl.multiple_of(j * cw, cw), cw)
        end_copy(i).wait_recv()
        for p, (lo, n) in enumerate(inward(i)):
            at = pl.ds(lo, n)
            out_ref[t, at, lanes] = add(sm[j, 0, at], r_end[j, 0, at], r_mid[j, 0, at]).astype(jnp.bfloat16)
            share(i, p)

    def finish_end(i):
        j = column(i)
        lanes = pl.ds(pl.multiple_of(j * cw, cw), cw)
        for p, ((lo, n), got) in enumerate(zip(inward(i), fin_copies(i))):
            at = pl.ds(lo, n)
            got.wait_recv()
            out_ref[t, at, lanes] = add(sm[j, 0, at], r_fin[j, at]).astype(jnp.bfloat16)
            share(i, p)

    def forward(i):
        for copies in share_copies(i):
            copies[0].wait_recv()
            copies[2].start()

    @pl.when(is_end)
    def _():
        down_chunk(0)
        settle(DOWN, 1)
        pair_sum(0)
        down_chunk(1)
        down_chunk(2)
        pair_sum(1)
        spread(DOWN, 3)
        pair_sum(2)
        end_rest(2)
        relay(DOWN, 2)
        settle(DOWN, 2)
        down_chunk(3)
        pair_sum(3)
        end_rest(3)
        relay(DOWN, 3)
        settle(DOWN, 3)
        down_chunk(4)
        down_chunk(5)
        pair_sum(4)
        pair_sum(5)

    @pl.when(is_mid)
    def _():
        settle(DOWN, 1)
        down_chunk(0)
        down_chunk(1)
        pair_sum(0)
        down_chunk(2)
        pair_sum(1)
        pair_sum(2)
        spread(DOWN, 2)
        spread(DOWN, 3)
        relay(DOWN, 2)
        pass_on(0)
        pass_on(1)
        relay(DOWN, 3)
        settle(DOWN, 2)
        down_chunk(3)
        pair_sum(3)
        pass_on(2)
        settle(DOWN, 3)
        down_chunk(4)
        down_chunk(5)
        pair_sum(4)
        pair_sum(5)

    def weights_sent(a):
        for k in range(4):
            if k > 0:
                z_copy(a, k).wait_send()
            for copy in across(a, k) + diagonal(a, k):
                copy.wait_send()

    def tokens_sent(mid):
        for k in range(4):
            token_pair(k).wait_send()
        for lane, (k, to, there) in enumerate(token_lanes(mid)):
            for s in range(strips):
                token_copy(lane, k, s, z_to(to), there).wait_send()

    def pairs_sent():
        for i in range(chunks):
            pair_copy(i).wait_send()

    @pl.when(is_mid)
    def _():
        hand_back(5)
        hand_back(4)
        pass_on(3)
        hand_back(3)
        finish_mid(3)
        weights_sent(GATE)
        pass_on(4)
        hand_back(2)
        finish_mid(2)
        pass_on(5)
        forward(3)
        hand_back(1)
        finish_mid(4)
        finish_mid(5)
        hand_back(0)
        forward(2)
        finish_mid(1)
        finish_mid(0)
        weights_sent(UP)
        weights_sent(DOWN)
        forward(4)
        tokens_sent(True)
        forward(5)
        pairs_sent()
        forward(1)
        forward(0)

    @pl.when(is_end)
    def _():
        end_rest(4, 5, 1, 0)
        finish_end(5)
        finish_end(4)
        weights_sent(GATE)
        forward(5)
        finish_end(3)
        forward(4)
        weights_sent(UP)
        weights_sent(DOWN)
        finish_end(2)
        forward(3)
        tokens_sent(False)
        finish_end(1)
        forward(2)
        pairs_sent()
        finish_end(0)
        forward(1)
        forward(0)

    def written(tt):
        return pltpu.make_async_copy(xs.at[tt], result_ref.at[tt], w_sem.at[tt])

    def complete_piece(tt):
        v = out_ref[tt].astype(jnp.float32)
        scale = lax.rsqrt(jnp.mean(v * v, axis=-1, keepdims=True) + epsilon)
        xs[tt] = (xs[tt].astype(jnp.float32) + v * scale * gains[1]).astype(jnp.bfloat16)
        written(tt).start()

    def take_shares(n):
        for i in range(chunks):
            for copies in share_copies(i):
                copies[n].wait_recv()

    complete_piece(t)
    complete_piece((t + 2) % 4)
    for n in (1, 2):
        take_shares(n)
        complete_piece((t + 1 - 2 * c + 2 * (n - 1)) % 4)
    for tt in range(4):
        written(tt).wait()
    for i in range(chunks):
        for copies in share_copies(i):
            for copy in copies:
                copy.wait_send()

    @pl.when(is_end)
    def _():
        for i in range(chunks):
            for copy in end_copies(i) + [end_copy(i)]:
                copy.wait_send()

    @pl.when(is_mid)
    def _():
        for i in range(chunks):
            for copy in mid_copies(i, outward(i)) + fin_copies(i):
                copy.wait_send()


def fused(tokens, norm_gain, gate_weight, up_weight, down_weight, branch_gain):
    rows, d = tokens.shape
    n_tp, planes = 4, 4
    rq = rows // n_tp
    hidden = gate_weight.shape[1]
    width = 2 * (hidden // planes)
    chunks = 2 * SUB
    cw = d // chunks
    bf16, f32, dma = jnp.bfloat16, jnp.float32, pltpu.SemaphoreType.DMA
    hbm = pl.BlockSpec(memory_space=pl.ANY)
    out = pl.pallas_call(
        kernel,
        out_shape=jax.ShapeDtypeStruct((n_tp, rq, d), bf16),
        in_specs=[hbm] * 6,
        out_specs=hbm,
        scratch_shapes=[
            pltpu.VMEM((n_tp, rq, d), bf16),
            pltpu.VMEM((2, 1, d), f32),
            pltpu.VMEM((n_tp, rq, d), bf16),
            pltpu.VMEM((planes, 2, rq, d), bf16),
            pltpu.VMEM((d, width), bf16),
            pltpu.VMEM((d, width), bf16),
            pltpu.VMEM((d, width), bf16),
            pltpu.VMEM((planes, 2 * rq, width), f32),
            pltpu.VMEM((planes, 2 * rq, width), bf16),
            pltpu.VMEM((chunks, planes, 2, rq, cw), bf16),
            pltpu.VMEM((chunks, planes, rq, cw), bf16),
            pltpu.VMEM((chunks, planes, rq, cw), bf16),
            pltpu.VMEM((chunks, 3, rq, cw), bf16),
            pltpu.VMEM((chunks, 2, rq, cw), bf16),
            pltpu.VMEM((chunks, rq, cw), bf16),
            dma((6,)),
            dma((3, 4)), dma((3, 4)),
            dma((3, 4)), dma((3, 4)),
            dma((3, 4)), dma((3, 4)),
            dma((3, 4)), dma((3, 4)),
            dma((3, 4)), dma((3, 4)),
            dma((5, rq // STRIP)), dma((4, rq // STRIP)),
            dma((4,)), dma((4,)),
            dma((chunks,)), dma((chunks,)),
            dma((chunks, 3)), dma((chunks, 3)),
            dma((chunks, 2)), dma((chunks, 2)),
            dma((chunks, 2)), dma((chunks, 2)),
            dma((chunks, 6)), dma((chunks, 6)),
            dma((n_tp,)),
        ],
        compiler_params=pltpu.CompilerParams(
            collective_id=0, has_side_effects=True, vmem_limit_bytes=60 * 1024 * 1024
        ),
    )(
        tokens.reshape(n_tp, rq, d), gate_weight, up_weight, down_weight.T, norm_gain, branch_gain,
    )
    return out.reshape(rows, d)


def solution(mesh):
    n_fs, n_tp = mesh.shape["fs"], mesh.shape["tp"]

    def per_device(*args):
        tokens, _, gate_weight = args[:3]
        rows, d = tokens.shape
        depth, hidden = gate_weight.shape
        fits = (
            n_fs == 8
            and n_tp == 4
            and rows % (STRIP * n_tp) == 0
            and depth % (2 * STRIP) == 0
            and hidden % (128 * 4) == 0
            and d % (128 * 2 * SUB) == 0
        )
        if fits:
            return fused(*args)
        return plain(*args)

    in_specs = (P("fs", None), P(), P("fs", "tp"), P("fs", "tp"), P("tp", "fs"), P())
    return jax.shard_map(
        per_device, mesh=mesh, in_specs=in_specs, out_specs=P("fs", None), check_vma=False
    )
```

```python
import functools

import jax
import jax.numpy as jnp
from jax import lax
from jax.experimental import pallas as pl
from jax.experimental.pallas import tpu as pltpu
from jax.sharding import PartitionSpec as P

MESH = pl.DeviceIdType.MESH
epsilon = 1e-06
GATE, UP, DOWN = 0, 1, 2
SUB = 3
STRIP = 16


def complete(own_tokens, summed, branch_gain):
    branch_scale = lax.rsqrt(jnp.mean(summed * summed, axis=-1, keepdims=True) + epsilon)
    return (own_tokens.astype(jnp.float32) + summed * branch_scale * branch_gain).astype(
        jnp.bfloat16
    )


def normalize(tokens, norm_gain):
    widened = tokens.astype(jnp.float32)
    scale = lax.rsqrt(jnp.mean(widened * widened, axis=-1, keepdims=True) + epsilon)
    return (widened * scale * norm_gain).astype(jnp.bfloat16)


def plain(tokens, norm_gain, gate_weight, up_weight, down_weight, branch_gain):
    normed = normalize(tokens, norm_gain)
    gate_whole, up_whole = (
        lax.all_gather(gate_weight, "fs", axis=0, tiled=True),
        lax.all_gather(up_weight, "fs", axis=0, tiled=True),
    )
    gate_sum = jnp.dot(normed, gate_whole, preferred_element_type=jnp.float32)
    up_sum = jnp.dot(normed, up_whole, preferred_element_type=jnp.float32)
    hidden = (jax.nn.silu(gate_sum) * up_sum).astype(jnp.bfloat16)
    partial_value = jnp.dot(
        hidden,
        lax.all_gather(down_weight, "fs", axis=1, tiled=True),
        preferred_element_type=jnp.float32,
    )
    summed = lax.psum(partial_value.astype(jnp.bfloat16), "tp").astype(jnp.float32)
    return complete(tokens, summed, branch_gain)


def kernel(tokens_ref, gate_ref, up_ref, down_ref, norm_gain_ref, branch_gain_ref, result_ref, *scratch):
    xs, gains, out_ref, xn, wg, wu, wd, gated, hid, part, pc, sm, r_end, r_mid, r_fin = scratch[:15]
    (loc_sem, sends_sem, w_send, t_send, z_recv, s_recv, d_recv, t_recv, td_recv, c_recv, e_recv, m_recv,
     f_recv, o_recv, oc_recv) = scratch[15:]
    f, t = lax.axis_index("fs"), lax.axis_index("tp")
    z, x, y, c = f // 2, f % 2, t // 2, t % 2
    h = z // 2
    middling = (z % 2 + z // 2) % 2
    is_mid, is_end = middling == 1, middling == 0
    plane = [z, z + 1 - 2 * (z % 2), 2 - h, 3 - 3 * h]
    slot = [0, 1, 3 - middling, 3 - middling]
    depth, width = gate_ref.shape[0], wg.shape[1] // 2
    rq, d = xn.shape[2:]
    strips = rq // STRIP
    chunks, cw = part.shape[0], part.shape[-1]
    rows = 8 * rq
    weights, inputs = (wg, wu, wd), (gate_ref, up_ref, down_ref)

    x_to, y_to, c_to = (f + 1 - 2 * x, t), (f, (t + 2) % 4), (f, t + 1 - 2 * c)
    yc_to = (f, (1 - y) * 2 + 1 - c)

    def z_to(k):
        return (plane[k] * 2 + x, t)

    barrier = pltpu.get_barrier_semaphore()
    for peer in (x_to, y_to, c_to, yc_to, z_to(1), z_to(2), z_to(3)):
        pl.semaphore_signal(barrier, inc=1, device_id=peer, device_id_type=MESH)

    def remote(src, dst, send, recv, to):
        return pltpu.make_async_remote_copy(
            src, dst, send, recv, device_id=to, device_id_type=MESH
        )

    def block(a, k, yy, lo=0, n=depth, flip=0):
        ff = plane[k] * 2 + (1 - x if flip else x)
        at = pl.ds(pl.multiple_of(ff * depth + lo, STRIP), n)
        return weights[a].at[at, pl.ds(pl.multiple_of(yy * width, width), width)]

    def quarter(a, k):
        return inputs[a].at[:, pl.ds(pl.multiple_of(plane[k] * width, width), width)]

    early = [
        pltpu.make_async_copy(tokens_ref, xs, loc_sem.at[3]),
        pltpu.make_async_copy(norm_gain_ref, gains.at[0, 0], loc_sem.at[4]),
        pltpu.make_async_copy(branch_gain_ref, gains.at[1, 0], loc_sem.at[5]),
    ]
    local = early + [
        pltpu.make_async_copy(quarter(a, 0), block(a, 0, y), loc_sem.at[a]) for a in range(3)
    ]
    for copy in local:
        copy.start()

    td_send, c_send, e_send, m_send, f_send, o_send, w_sem = (sends_sem.at[i] for i in range(7))

    def stretch(a, n):
        return weights[a].at[pl.ds(0, n * depth), pl.ds(0, width)]

    def wait_sent(piece, sem):
        remote(piece, piece, sem, oc_recv.at[0], c_to).wait_send()

    def wait_got(piece, sem):
        remote(piece, piece, w_sem, sem, c_to).wait_recv()

    def z_copy(a, k):
        return remote(
            quarter(a, k), block(a, 0, y), w_send.at[a, 0], z_recv.at[a, slot[k]], z_to(k)
        )

    def z_wait(a, k):
        wait_got(stretch(a, 1), z_recv.at[a, k])

    def across(a, k):
        src = quarter(a, 0) if k == 0 else block(a, k, y)
        return (
            remote(src, block(a, k, y), w_send.at[a, 1], s_recv.at[a, k], x_to),
            remote(src, block(a, k, y), w_send.at[a, 1], s_recv.at[a, k], y_to),
        )

    def diagonal(a, k):
        n = depth // 2
        first, second = block(a, k, y, 0, n, 1), block(a, k, 1 - y, n, n)
        return (
            remote(first, first, w_send.at[a, 2], d_recv.at[a, k], y_to),
            remote(second, second, w_send.at[a, 2], d_recv.at[a, k], x_to),
        )

    def spread(a, k):
        if k > 0:
            z_wait(a, k)
        for copy in across(a, k):
            copy.start()

    def relay(a, k):
        wait_got(stretch(a, 2), s_recv.at[a, k])
        for copy in diagonal(a, k):
            copy.start()

    def settle(a, k):
        wait_got(stretch(a, 1), d_recv.at[a, k])

    def strip(k, s):
        return xn.at[plane[k], c, pl.ds(s * STRIP, STRIP)]

    def token_copy(lane, k, s, to, slot):
        piece = strip(k, s)
        return remote(piece, piece, t_send.at[lane], t_recv.at[slot - 1, s], to)

    def token_wait(k, s):
        wait_got(strip(k, s), t_recv.at[k - 1, s])

    def token_pair(k):
        piece = xn.at[plane[k], c]
        return remote(piece, piece, td_send, td_recv.at[k], c_to)

    def token_lanes(mid):
        if mid:
            return [(0, 1, 1), (0, 2, 2), (1, 2, 3), (2, 1, 2), (3, 1, 3)]
        return [(0, 1, 1)]

    def token_relay(mid, lane, lo=0, hi=strips):
        k, to, there = token_lanes(mid)[lane]
        for s in range(lo, hi):
            if k > 0:
                token_wait(k, s)
            token_copy(lane, k, s, z_to(to), there).start()
        if k > 0 and hi == strips:
            token_pair(k).start()

    def token_take(k):
        for s in range(strips):
            token_wait(k, s)
        token_pair(k).start()

    def token_settle(*which):
        for k in which:
            wait_got(xn.at[0, 0], td_recv.at[k])

    pl.semaphore_wait(barrier, 7)

    def sends(*pairs):
        for a, k in pairs:
            z_copy(a, k).start()

    @pl.when(is_end)
    def _():
        sends((GATE, 1), (GATE, 2), (GATE, 3), (UP, 1), (UP, 2), (UP, 3))

    @pl.when(is_mid)
    def _():
        sends((GATE, 2), (GATE, 1), (GATE, 3), (UP, 2), (UP, 1), (UP, 3))

    spread(GATE, 0)
    spread(UP, 0)

    for copy in early:
        copy.wait()
    for s in range(strips):
        at_rows = pl.ds(s * STRIP, STRIP)
        v = xs[t, at_rows, :].astype(jnp.float32)
        scale = lax.rsqrt(jnp.mean(v * v, axis=-1, keepdims=True) + epsilon)
        xn[z, c, at_rows, :] = (v * scale * gains[0]).astype(jnp.bfloat16)
    token_pair(0).start()

    @pl.when(is_end)
    def _():
        token_relay(False, 0)
        sends((DOWN, 1))

    @pl.when(is_mid)
    def _():
        token_relay(True, 1)
        token_relay(True, 0)

    def product(w, zb, nb, n0, nw):
        v = xn[pl.ds(zb, nb)].reshape(nb * 2 * rq, d)
        return jnp.dot(
            v, w[:, pl.ds(pl.multiple_of(n0, nw), nw)], preferred_element_type=jnp.float32
        )

    def gate_rows(zb, nb):
        def one(i, carry):
            n0 = pl.multiple_of(i * width, width)
            v = product(wg, zb, nb, n0, width)
            v = v / (1.0 + jnp.exp(-v))
            gated[pl.ds(zb, nb), :, pl.ds(n0, width)] = v.reshape(nb, 2 * rq, width)
            return carry

        lax.fori_loop(0, 2, one, 0)

    def up_rows(zb, nb):
        def one(i, carry):
            n0 = pl.multiple_of(i * width, width)
            v = product(wu, zb, nb, n0, width).reshape(nb, 2 * rq, width)
            v = gated[pl.ds(zb, nb), :, pl.ds(n0, width)] * v
            hid[pl.ds(zb, nb), :, pl.ds(n0, width)] = v.astype(jnp.bfloat16)
            return carry

        lax.fori_loop(0, 2, one, 0)

    def settle_all(a):
        for k in range(4):
            settle(a, k)

    def own_weights():
        for copy in local[3:]:
            copy.wait()

    @pl.when(is_end)
    def _():
        relay(GATE, 0)
        spread(GATE, 1)
        relay(UP, 0)
        spread(UP, 1)
        relay(GATE, 1)
        spread(GATE, 2)
        relay(UP, 1)
        spread(GATE, 3)
        relay(GATE, 2)
        spread(UP, 2)
        relay(GATE, 3)
        spread(UP, 3)
        relay(UP, 2)
        token_take(1)
        relay(UP, 3)
        spread(DOWN, 0)
        settle_all(GATE)
        own_weights()
        token_settle(0, 1)
        gate_rows(h * 2, 2)
        settle_all(UP)
        up_rows(h * 2, 2)
        sends((DOWN, 3), (DOWN, 2))
        token_take(2)
        relay(DOWN, 0)
        token_settle(2)
        gate_rows(plane[2], 1)
        up_rows(plane[2], 1)
        spread(DOWN, 1)
        token_take(3)
        token_settle(3)
        gate_rows(plane[3], 1)
        relay(DOWN, 1)
        up_rows(plane[3], 1)
        spread(DOWN, 2)
        settle(DOWN, 0)

    @pl.when(is_mid)
    def _():
        relay(GATE, 0)
        spread(GATE, 1)
        relay(UP, 0)
        spread(GATE, 2)
        relay(GATE, 1)
        spread(GATE, 3)
        spread(UP, 1)
        relay(GATE, 2)
        spread(UP, 2)
        relay(GATE, 3)
        relay(UP, 1)
        spread(UP, 3)
        sends((DOWN, 1))
        token_relay(True, 2)
        token_relay(True, 3, 0, 3)
        relay(UP, 2)
        token_relay(True, 3, 3)
        token_relay(True, 4, 0, 4)
        relay(UP, 3)
        spread(DOWN, 0)
        settle_all(GATE)
        own_weights()
        token_settle(0, 1)
        gate_rows(h * 2, 2)
        token_relay(True, 4, 4)
        sends((DOWN, 3), (DOWN, 2))
        settle_all(UP)
        up_rows(h * 2, 2)
        relay(DOWN, 0)
        spread(DOWN, 1)
        token_settle(2)
        gate_rows(plane[2], 1)
        up_rows(plane[2], 1)
        relay(DOWN, 1)
        token_settle(3)
        gate_rows(plane[3], 1)
        up_rows(plane[3], 1)
        settle(DOWN, 0)

    def column(i):
        return h * (chunks - 1) + (1 - 2 * h) * i

    def pair_copy(i):
        j = column(i)
        return remote(part.at[j, :, 1 - c], pc.at[j], c_send, c_recv.at[j], c_to)

    def down_chunk(i):
        j = column(i)
        value = lax.dot_general(
            hid[...].reshape(rows, 2 * width), wd[pl.ds(pl.multiple_of(j * cw, cw), cw), :], (((1,), (1,)), ((), ())),
            preferred_element_type=jnp.float32,
        ).astype(jnp.bfloat16)
        for zz in range(4):
            for cc in range(2):
                at = (zz * 2 + cc) * rq
                part[j, zz, cc] = value[at:at + rq]
        pair_copy(i).start()

    def add(*terms):
        return functools.reduce(lambda a, b: a + b, [v.astype(jnp.float32) for v in terms])

    first = (rq // STRIP + 1) // 2 * STRIP
    whole, halves = [(0, rq)], [(0, first), (first, rq - first)]

    def outward(i):
        return halves if i >= chunks - 2 else whole

    def inward(i):
        return halves if i < 2 else whole

    def end_copies(i):
        j = column(i)
        return [
            remote(
                sm.at[j, pl.ds(2, 2), pl.ds(lo, n)], r_end.at[j, pl.ds(1, 2), pl.ds(lo, n)],
                e_send, e_recv.at[j, p], z_to(1),
            )
            for p, (lo, n) in enumerate(outward(i))
        ]

    def end_copy(i):
        j = column(i)
        return remote(sm.at[j, 1], r_end.at[j, 0], e_send, e_recv.at[j, 2], z_to(1))

    def mid_copies(i, parts):
        j = column(i)
        return [
            remote(
                sm.at[j, pl.ds(2, 2), pl.ds(lo, n)], r_mid.at[j, :, pl.ds(lo, n)],
                m_send, m_recv.at[j, p], z_to(2),
            )
            for p, (lo, n) in enumerate(parts)
        ]

    def fin_copies(i):
        j = column(i)
        return [
            remote(
                sm.at[j, 1, pl.ds(lo, n)], r_fin.at[j, pl.ds(lo, n)],
                f_send, f_recv.at[j, p], z_to(1),
            )
            for p, (lo, n) in enumerate(inward(i))
        ]

    def pair_sum(i):
        pair_copy(i).wait_recv()
        j = column(i)
        for k in range(4):
            sm[j, k] = add(part[j, plane[k], c], pc[j, plane[k]]).astype(jnp.bfloat16)

        @pl.when(is_end)
        def _():
            for copy in end_copies(i):
                copy.start()

    def end_rest(*which):
        for i in which:
            end_copy(i).start()

    def pass_on(i):
        j = column(i)
        for (lo, n), got, on in zip(outward(i), end_copies(i), mid_copies(i, outward(i))):
            at = pl.ds(lo, n)
            got.wait_recv()
            sm[j, 2, at] = add(sm[j, 2, at], r_end[j, 1, at]).astype(jnp.bfloat16)
            sm[j, 3, at] = add(sm[j, 3, at], r_end[j, 2, at]).astype(jnp.bfloat16)
            on.start()

    def share_copies(i):
        j = column(i)
        lanes = pl.ds(pl.multiple_of(j * cw, cw), cw)
        every = []
        for p, (lo, n) in enumerate(inward(i)):
            own, other = out_ref.at[t, pl.ds(lo, n), lanes], out_ref.at[(t + 2) % 4, pl.ds(lo, n), lanes]
            every.append([
                remote(own, own, o_send, o_recv.at[j, p], y_to),
                remote(own, own, o_send, oc_recv.at[0], c_to),
                remote(other, other, o_send, oc_recv.at[1], c_to),
            ])
        return every

    def share(i, p):
        for copy in share_copies(i)[p][:2]:
            copy.start()

    def hand_back(i):
        j = column(i)
        for (lo, n), got, on in zip(inward(i), mid_copies(i, inward(i)), fin_copies(i)):
            at = pl.ds(lo, n)
            got.wait_recv()
            sm[j, 1, at] = add(sm[j, 1, at], r_mid[j, 1, at]).astype(jnp.bfloat16)
            on.start()

    def finish_mid(i):
        j = column(i)
        lanes = pl.ds(pl.multiple_of(j * cw, cw), cw)
        end_copy(i).wait_recv()
        for p, (lo, n) in enumerate(inward(i)):
            at = pl.ds(lo, n)
            out_ref[t, at, lanes] = add(sm[j, 0, at], r_end[j, 0, at], r_mid[j, 0, at]).astype(jnp.bfloat16)
            share(i, p)

    def finish_end(i):
        j = column(i)
        lanes = pl.ds(pl.multiple_of(j * cw, cw), cw)
        for p, ((lo, n), got) in enumerate(zip(inward(i), fin_copies(i))):
            at = pl.ds(lo, n)
            got.wait_recv()
            out_ref[t, at, lanes] = add(sm[j, 0, at], r_fin[j, at]).astype(jnp.bfloat16)
            share(i, p)

    def forward(i):
        for copies in share_copies(i):
            copies[0].wait_recv()
            copies[2].start()

    @pl.when(is_end)
    def _():
        down_chunk(0)
        settle(DOWN, 1)
        pair_sum(0)
        down_chunk(1)
        down_chunk(2)
        pair_sum(1)
        spread(DOWN, 3)
        pair_sum(2)
        end_rest(2)
        relay(DOWN, 2)
        settle(DOWN, 2)
        down_chunk(3)
        pair_sum(3)
        end_rest(3)
        relay(DOWN, 3)
        settle(DOWN, 3)
        down_chunk(4)
        down_chunk(5)
        pair_sum(4)
        pair_sum(5)

    @pl.when(is_mid)
    def _():
        settle(DOWN, 1)
        down_chunk(0)
        down_chunk(1)
        pair_sum(0)
        down_chunk(2)
        pair_sum(1)
        pair_sum(2)
        spread(DOWN, 2)
        spread(DOWN, 3)
        relay(DOWN, 2)
        pass_on(0)
        pass_on(1)
        relay(DOWN, 3)
        settle(DOWN, 2)
        down_chunk(3)
        pair_sum(3)
        pass_on(2)
        settle(DOWN, 3)
        down_chunk(4)
        down_chunk(5)
        pair_sum(4)
        pair_sum(5)

    def weights_sent(a):
        wait_sent(stretch(a, 3), w_send.at[a, 0])
        wait_sent(stretch(a, 8), w_send.at[a, 1])
        wait_sent(stretch(a, 4), w_send.at[a, 2])

    def tokens_sent(mid):
        wait_sent(xn.at[:, 0], td_send)
        for lane in range(len(token_lanes(mid))):
            wait_sent(xn.at[0, 0], t_send.at[lane])

    def pairs_sent():
        wait_sent(pc, c_send)

    @pl.when(is_mid)
    def _():
        hand_back(5)
        hand_back(4)
        pass_on(3)
        hand_back(3)
        finish_mid(3)
        weights_sent(GATE)
        pass_on(4)
        hand_back(2)
        finish_mid(2)
        pass_on(5)
        forward(3)
        hand_back(1)
        finish_mid(4)
        finish_mid(5)
        hand_back(0)
        forward(2)
        finish_mid(1)
        finish_mid(0)
        weights_sent(UP)
        weights_sent(DOWN)
        forward(4)
        tokens_sent(True)
        forward(5)
        pairs_sent()
        forward(1)
        forward(0)

    @pl.when(is_end)
    def _():
        end_rest(4, 5, 1, 0)
        finish_end(5)
        finish_end(4)
        weights_sent(GATE)
        forward(5)
        finish_end(3)
        forward(4)
        weights_sent(UP)
        weights_sent(DOWN)
        finish_end(2)
        forward(3)
        tokens_sent(False)
        finish_end(1)
        forward(2)
        pairs_sent()
        finish_end(0)
        forward(1)
        forward(0)

    def complete_piece(tt):
        v = out_ref[tt].astype(jnp.float32)
        scale = lax.rsqrt(jnp.mean(v * v, axis=-1, keepdims=True) + epsilon)
        xs[tt] = (xs[tt].astype(jnp.float32) + v * scale * gains[1]).astype(jnp.bfloat16)
        pltpu.make_async_copy(xs.at[tt], result_ref.at[tt], w_sem).start()

    complete_piece(t)
    complete_piece((t + 2) % 4)
    for n in range(2):
        wait_got(out_ref.at[0], oc_recv.at[n])
        complete_piece((t + 1 - 2 * c + 2 * n) % 4)
    wait_sent(out_ref.at[pl.ds(0, 3)], o_send)

    @pl.when(is_end)
    def _():
        wait_sent(r_end, e_send)

    @pl.when(is_mid)
    def _():
        wait_sent(r_mid, m_send)
        wait_sent(r_fin, f_send)

    pltpu.make_async_copy(xs, result_ref, w_sem).wait()


def fused(tokens, norm_gain, gate_weight, up_weight, down_weight, branch_gain):
    rows, d = tokens.shape
    n_tp, planes = 4, 4
    rq = rows // n_tp
    hidden = gate_weight.shape[1]
    width = 2 * (hidden // planes)
    chunks = 2 * SUB
    cw = d // chunks
    bf16, f32, dma = jnp.bfloat16, jnp.float32, pltpu.SemaphoreType.DMA
    hbm = pl.BlockSpec(memory_space=pl.ANY)
    out = pl.pallas_call(
        kernel,
        out_shape=jax.ShapeDtypeStruct((n_tp, rq, d), bf16),
        in_specs=[hbm] * 6,
        out_specs=hbm,
        scratch_shapes=[
            pltpu.VMEM((n_tp, rq, d), bf16),
            pltpu.VMEM((2, 1, d), f32),
            pltpu.VMEM((n_tp, rq, d), bf16),
            pltpu.VMEM((planes, 2, rq, d), bf16),
            pltpu.VMEM((d, width), bf16),
            pltpu.VMEM((d, width), bf16),
            pltpu.VMEM((d, width), bf16),
            pltpu.VMEM((planes, 2 * rq, width), f32),
            pltpu.VMEM((planes, 2 * rq, width), bf16),
            pltpu.VMEM((chunks, planes, 2, rq, cw), bf16),
            pltpu.VMEM((chunks, planes, rq, cw), bf16),
            pltpu.VMEM((chunks, planes, rq, cw), bf16),
            pltpu.VMEM((chunks, 3, rq, cw), bf16),
            pltpu.VMEM((chunks, 2, rq, cw), bf16),
            pltpu.VMEM((chunks, rq, cw), bf16),
            dma((6,)), dma((7,)), dma((3, 3)), dma((5,)),
            dma((3, 4)), dma((3, 4)), dma((3, 4)),
            dma((3, rq // STRIP)), dma((4,)), dma((chunks,)),
            dma((chunks, 3)), dma((chunks, 2)), dma((chunks, 2)), dma((chunks, 2)), dma((2,)),
        ],
        compiler_params=pltpu.CompilerParams(
            collective_id=0, has_side_effects=True, vmem_limit_bytes=60 * 1024 * 1024
        ),
    )(
        tokens.reshape(n_tp, rq, d), gate_weight, up_weight, down_weight.T, norm_gain, branch_gain,
    )
    return out.reshape(rows, d)


def solution(mesh):
    n_fs, n_tp = mesh.shape["fs"], mesh.shape["tp"]

    def per_device(*args):
        tokens, _, gate_weight = args[:3]
        rows, d = tokens.shape
        depth, hidden = gate_weight.shape
        fits = (
            n_fs == 8
            and n_tp == 4
            and rows % (STRIP * n_tp) == 0
            and depth % (2 * STRIP) == 0
            and hidden % (128 * 4) == 0
            and d % (128 * 2 * SUB) == 0
        )
        if fits:
            return fused(*args)
        return plain(*args)

    in_specs = (P("fs", None), P(), P("fs", "tp"), P("fs", "tp"), P("tp", "fs"), P())
    return jax.shard_map(
        per_device, mesh=mesh, in_specs=in_specs, out_specs=P("fs", None), check_vma=False
    )
```

```python
import functools

import jax
import jax.numpy as jnp
from jax import lax
from jax.experimental import pallas as pl
from jax.experimental.pallas import tpu as pltpu
from jax.sharding import PartitionSpec as P

MESH = pl.DeviceIdType.MESH
epsilon = 1e-06
GATE, UP, DOWN = 0, 1, 2
SUB = 3
STRIP = 16


def complete(own_tokens, summed, branch_gain):
    branch_scale = lax.rsqrt(jnp.mean(summed * summed, axis=-1, keepdims=True) + epsilon)
    return (own_tokens.astype(jnp.float32) + summed * branch_scale * branch_gain).astype(
        jnp.bfloat16
    )


def normalize(tokens, norm_gain):
    widened = tokens.astype(jnp.float32)
    scale = lax.rsqrt(jnp.mean(widened * widened, axis=-1, keepdims=True) + epsilon)
    return (widened * scale * norm_gain).astype(jnp.bfloat16)


def plain(tokens, norm_gain, gate_weight, up_weight, down_weight, branch_gain):
    normed = normalize(tokens, norm_gain)
    gate_whole, up_whole = (
        lax.all_gather(gate_weight, "fs", axis=0, tiled=True),
        lax.all_gather(up_weight, "fs", axis=0, tiled=True),
    )
    gate_sum = jnp.dot(normed, gate_whole, preferred_element_type=jnp.float32)
    up_sum = jnp.dot(normed, up_whole, preferred_element_type=jnp.float32)
    hidden = (jax.nn.silu(gate_sum) * up_sum).astype(jnp.bfloat16)
    partial_value = jnp.dot(
        hidden,
        lax.all_gather(down_weight, "fs", axis=1, tiled=True),
        preferred_element_type=jnp.float32,
    )
    summed = lax.psum(partial_value.astype(jnp.bfloat16), "tp").astype(jnp.float32)
    return complete(tokens, summed, branch_gain)


def kernel(tokens_ref, gate_ref, up_ref, down_ref, norm_gain_ref, branch_gain_ref, result_ref, *scratch):
    xs, gains, out_ref, xn, wg, wu, wd, gated, hid, part, pc, sm, r_end, r_mid, r_fin = scratch[:15]
    (loc_sem, sends_sem, w_send, t_send, z_recv, s_recv, d_recv, t_recv, td_recv, c_recv, e_recv, m_recv,
     f_recv, o_recv, oc_recv) = scratch[15:]
    f, t = lax.axis_index("fs"), lax.axis_index("tp")
    z, x, y, c = f // 2, f % 2, t // 2, t % 2
    h = z // 2
    middling = (z % 2 + z // 2) % 2
    is_mid, is_end = middling == 1, middling == 0
    plane = [z, z + 1 - 2 * (z % 2), 2 - h, 3 - 3 * h]
    slot = [0, 1, 3 - middling, 3 - middling]
    depth, width = gate_ref.shape[0], wg.shape[1] // 2
    rq, d = xn.shape[2:]
    strips = rq // STRIP
    chunks, cw = part.shape[0], part.shape[-1]
    rows = 8 * rq
    weights, inputs = (wg, wu, wd), (gate_ref, up_ref, down_ref)

    x_to, y_to, c_to = (f + 1 - 2 * x, t), (f, (t + 2) % 4), (f, t + 1 - 2 * c)
    yc_to = (f, (1 - y) * 2 + 1 - c)

    def z_to(k):
        return (plane[k] * 2 + x, t)

    barrier = pltpu.get_barrier_semaphore()
    for peer in (x_to, y_to, c_to, yc_to, z_to(1), z_to(2), z_to(3)):
        pl.semaphore_signal(barrier, inc=1, device_id=peer, device_id_type=MESH)

    def remote(src, dst, send, recv, to):
        return pltpu.make_async_remote_copy(
            src, dst, send, recv, device_id=to, device_id_type=MESH
        )

    def block(a, k, yy, lo=0, n=depth, flip=0):
        ff = plane[k] * 2 + (1 - x if flip else x)
        at = pl.ds(pl.multiple_of(ff * depth + lo, STRIP), n)
        return weights[a].at[at, pl.ds(pl.multiple_of(yy * width, width), width)]

    def quarter(a, k):
        return inputs[a].at[:, pl.ds(pl.multiple_of(plane[k] * width, width), width)]

    early = [
        pltpu.make_async_copy(tokens_ref, xs, loc_sem.at[3]),
        pltpu.make_async_copy(norm_gain_ref, gains.at[0, 0], loc_sem.at[4]),
        pltpu.make_async_copy(branch_gain_ref, gains.at[1, 0], loc_sem.at[5]),
    ]
    local = early + [
        pltpu.make_async_copy(quarter(a, 0), block(a, 0, y), loc_sem.at[a]) for a in range(3)
    ]
    for copy in local:
        copy.start()

    td_send, c_send, e_send, m_send, f_send, o_send, w_sem = (sends_sem.at[i] for i in range(7))

    def stretch(a, n):
        return weights[a].at[pl.ds(0, n * depth), pl.ds(0, width)]

    def wait_sent(piece, sem):
        remote(piece, piece, sem, oc_recv.at[0], c_to).wait_send()

    def wait_got(piece, sem):
        remote(piece, piece, w_sem, sem, c_to).wait_recv()

    def z_copy(a, k):
        return remote(
            quarter(a, k), block(a, 0, y), w_send.at[a, 0], z_recv.at[a, slot[k]], z_to(k)
        )

    def z_wait(a, k):
        wait_got(stretch(a, 1), z_recv.at[a, k])

    def across(a, k):
        src = quarter(a, 0) if k == 0 else block(a, k, y)
        return (
            remote(src, block(a, k, y), w_send.at[a, 1], s_recv.at[a, k], x_to),
            remote(src, block(a, k, y), w_send.at[a, 1], s_recv.at[a, k], y_to),
        )

    def diagonal(a, k):
        n = depth // 2
        first, second = block(a, k, y, 0, n, 1), block(a, k, 1 - y, n, n)
        return (
            remote(first, first, w_send.at[a, 2], d_recv.at[a, k], y_to),
            remote(second, second, w_send.at[a, 2], d_recv.at[a, k], x_to),
        )

    def spread(a, k):
        if k > 0:
            z_wait(a, k)
        for copy in across(a, k):
            copy.start()

    def relay(a, k):
        wait_got(stretch(a, 2), s_recv.at[a, k])
        for copy in diagonal(a, k):
            copy.start()

    def settle(a, k):
        wait_got(stretch(a, 1), d_recv.at[a, k])

    def strip(k, s):
        return xn.at[plane[k], c, pl.ds(s * STRIP, STRIP)]

    def token_copy(lane, k, s, to, slot):
        piece = strip(k, s)
        return remote(piece, piece, t_send.at[lane], t_recv.at[slot - 1, s], to)

    def token_wait(k, s):
        wait_got(strip(k, s), t_recv.at[k - 1, s])

    def token_pair(k):
        piece = xn.at[plane[k], c]
        return remote(piece, piece, td_send, td_recv.at[k], c_to)

    def token_lanes(mid):
        if mid:
            return [(0, 1, 1), (0, 2, 2), (1, 2, 3), (2, 1, 2), (3, 1, 3)]
        return [(0, 1, 1)]

    def token_relay(mid, lane, lo=0, hi=strips):
        k, to, there = token_lanes(mid)[lane]
        for s in range(lo, hi):
            if k > 0:
                token_wait(k, s)
            token_copy(lane, k, s, z_to(to), there).start()
        if k > 0 and hi == strips:
            token_pair(k).start()

    def token_take(k):
        for s in range(strips):
            token_wait(k, s)
        token_pair(k).start()

    def token_settle(*which):
        for k in which:
            wait_got(xn.at[0, 0], td_recv.at[k])

    pl.semaphore_wait(barrier, 7)

    def sends(*pairs):
        for a, k in pairs:
            z_copy(a, k).start()

    @pl.when(is_end)
    def _():
        sends((GATE, 1), (GATE, 2), (GATE, 3), (UP, 1), (UP, 2), (UP, 3))

    @pl.when(is_mid)
    def _():
        sends((GATE, 2), (GATE, 1), (GATE, 3), (UP, 2), (UP, 1), (UP, 3))

    spread(GATE, 0)
    spread(UP, 0)

    for copy in early:
        copy.wait()
    for s in range(strips):
        at_rows = pl.ds(s * STRIP, STRIP)
        v = xs[t, at_rows, :].astype(jnp.float32)
        scale = lax.rsqrt(jnp.mean(v * v, axis=-1, keepdims=True) + epsilon)
        xn[z, c, at_rows, :] = (v * scale * gains[0]).astype(jnp.bfloat16)
    token_pair(0).start()

    @pl.when(is_end)
    def _():
        token_relay(False, 0)
        sends((DOWN, 1))

    @pl.when(is_mid)
    def _():
        token_relay(True, 1)
        token_relay(True, 0)

    def product(w, zb, nb, n0, nw):
        v = xn[pl.ds(zb, nb)].reshape(nb * 2 * rq, d)
        return jnp.dot(
            v, w[:, pl.ds(pl.multiple_of(n0, nw), nw)], preferred_element_type=jnp.float32
        )

    def gate_rows(zb, nb):
        def one(i, carry):
            n0 = pl.multiple_of(i * width, width)
            v = product(wg, zb, nb, n0, width)
            v = v / (1.0 + jnp.exp(-v))
            gated[pl.ds(zb, nb), :, pl.ds(n0, width)] = v.reshape(nb, 2 * rq, width)
            return carry

        lax.fori_loop(0, 2, one, 0)

    def up_rows(zb, nb):
        def one(i, carry):
            n0 = pl.multiple_of(i * width, width)
            v = product(wu, zb, nb, n0, width).reshape(nb, 2 * rq, width)
            v = gated[pl.ds(zb, nb), :, pl.ds(n0, width)] * v
            hid[pl.ds(zb, nb), :, pl.ds(n0, width)] = v.astype(jnp.bfloat16)
            return carry

        lax.fori_loop(0, 2, one, 0)

    def settle_all(a):
        for k in range(4):
            settle(a, k)

    def own_weights():
        for copy in local[3:]:
            copy.wait()

    @pl.when(is_end)
    def _():
        relay(GATE, 0)
        spread(GATE, 1)
        relay(UP, 0)
        spread(UP, 1)
        relay(GATE, 1)
        spread(GATE, 2)
        relay(UP, 1)
        spread(GATE, 3)
        relay(GATE, 2)
        spread(UP, 2)
        relay(GATE, 3)
        spread(UP, 3)
        relay(UP, 2)
        token_take(1)
        relay(UP, 3)
        spread(DOWN, 0)
        settle_all(GATE)
        own_weights()
        token_settle(0, 1)
        gate_rows(h * 2, 2)
        settle_all(UP)
        up_rows(h * 2, 2)
        sends((DOWN, 3), (DOWN, 2))
        token_take(2)
        relay(DOWN, 0)
        token_settle(2)
        gate_rows(plane[2], 1)
        up_rows(plane[2], 1)
        spread(DOWN, 1)
        token_take(3)
        token_settle(3)
        gate_rows(plane[3], 1)
        relay(DOWN, 1)
        up_rows(plane[3], 1)
        spread(DOWN, 2)
        settle(DOWN, 0)

    @pl.when(is_mid)
    def _():
        relay(GATE, 0)
        spread(GATE, 1)
        relay(UP, 0)
        spread(GATE, 2)
        relay(GATE, 1)
        spread(GATE, 3)
        spread(UP, 1)
        relay(GATE, 2)
        spread(UP, 2)
        relay(GATE, 3)
        relay(UP, 1)
        spread(UP, 3)
        sends((DOWN, 1))
        token_relay(True, 2)
        token_relay(True, 3, 0, 3)
        relay(UP, 2)
        token_relay(True, 3, 3)
        token_relay(True, 4, 0, 4)
        relay(UP, 3)
        spread(DOWN, 0)
        settle_all(GATE)
        own_weights()
        token_settle(0, 1)
        gate_rows(h * 2, 2)
        token_relay(True, 4, 4)
        sends((DOWN, 3), (DOWN, 2))
        settle_all(UP)
        up_rows(h * 2, 2)
        relay(DOWN, 0)
        spread(DOWN, 1)
        token_settle(2)
        gate_rows(plane[2], 1)
        up_rows(plane[2], 1)
        relay(DOWN, 1)
        token_settle(3)
        gate_rows(plane[3], 1)
        up_rows(plane[3], 1)
        settle(DOWN, 0)

    def column(i):
        return h * (chunks - 1) + (1 - 2 * h) * i

    def pair_copy(i):
        j = column(i)
        return remote(part.at[j, :, 1 - c], pc.at[j], c_send, c_recv.at[j], c_to)

    def down_chunk(i):
        j = column(i)
        value = lax.dot_general(
            hid[...].reshape(rows, 2 * width), wd[pl.ds(pl.multiple_of(j * cw, cw), cw), :], (((1,), (1,)), ((), ())),
            preferred_element_type=jnp.float32,
        ).astype(jnp.bfloat16)
        for zz in range(4):
            for cc in range(2):
                at = (zz * 2 + cc) * rq
                part[j, zz, cc] = value[at:at + rq]
        pair_copy(i).start()

    def add(*terms):
        return functools.reduce(lambda a, b: a + b, [v.astype(jnp.float32) for v in terms])

    first = (rq // STRIP + 1) // 2 * STRIP
    whole, halves = [(0, rq)], [(0, first), (first, rq - first)]

    def outward(i):
        return halves if i >= chunks - 2 else whole

    def inward(i):
        return halves if i < 2 else whole

    def end_copies(i):
        j = column(i)
        return [
            remote(
                sm.at[j, pl.ds(2, 2), pl.ds(lo, n)], r_end.at[j, pl.ds(1, 2), pl.ds(lo, n)],
                e_send, e_recv.at[j, p], z_to(1),
            )
            for p, (lo, n) in enumerate(outward(i))
        ]

    def end_copy(i):
        j = column(i)
        return remote(sm.at[j, 1], r_end.at[j, 0], e_send, e_recv.at[j, 2], z_to(1))

    def mid_copies(i, parts):
        j = column(i)
        return [
            remote(
                sm.at[j, pl.ds(2, 2), pl.ds(lo, n)], r_mid.at[j, :, pl.ds(lo, n)],
                m_send, m_recv.at[j, p], z_to(2),
            )
            for p, (lo, n) in enumerate(parts)
        ]

    def fin_copies(i):
        j = column(i)
        return [
            remote(
                sm.at[j, 1, pl.ds(lo, n)], r_fin.at[j, pl.ds(lo, n)],
                f_send, f_recv.at[j, p], z_to(1),
            )
            for p, (lo, n) in enumerate(inward(i))
        ]

    def pair_sum(i):
        pair_copy(i).wait_recv()
        j = column(i)
        for k in range(4):
            sm[j, k] = add(part[j, plane[k], c], pc[j, plane[k]]).astype(jnp.bfloat16)

        @pl.when(is_end)
        def _():
            for copy in end_copies(i):
                copy.start()

    def end_rest(*which):
        for i in which:
            end_copy(i).start()

    def pass_on(i):
        j = column(i)
        for (lo, n), got, on in zip(outward(i), end_copies(i), mid_copies(i, outward(i))):
            at = pl.ds(lo, n)
            got.wait_recv()
            sm[j, 2, at] = add(sm[j, 2, at], r_end[j, 1, at]).astype(jnp.bfloat16)
            sm[j, 3, at] = add(sm[j, 3, at], r_end[j, 2, at]).astype(jnp.bfloat16)
            on.start()

    def share_copies(i):
        j = column(i)
        lanes = pl.ds(pl.multiple_of(j * cw, cw), cw)
        every = []
        for p, (lo, n) in enumerate(inward(i)):
            own, other = out_ref.at[t, pl.ds(lo, n), lanes], out_ref.at[(t + 2) % 4, pl.ds(lo, n), lanes]
            every.append([
                remote(own, own, o_send, o_recv.at[j, p], y_to),
                remote(own, own, o_send, oc_recv.at[0], c_to),
                remote(other, other, o_send, oc_recv.at[1], c_to),
            ])
        return every

    def share(i, p):
        for copy in share_copies(i)[p][:2]:
            copy.start()

    def hand_back(i):
        j = column(i)
        for (lo, n), got, on in zip(inward(i), mid_copies(i, inward(i)), fin_copies(i)):
            at = pl.ds(lo, n)
            got.wait_recv()
            sm[j, 1, at] = add(sm[j, 1, at], r_mid[j, 1, at]).astype(jnp.bfloat16)
            on.start()

    def finish_mid(i):
        j = column(i)
        lanes = pl.ds(pl.multiple_of(j * cw, cw), cw)
        end_copy(i).wait_recv()
        for p, (lo, n) in enumerate(inward(i)):
            at = pl.ds(lo, n)
            out_ref[t, at, lanes] = add(sm[j, 0, at], r_end[j, 0, at], r_mid[j, 0, at]).astype(jnp.bfloat16)
            share(i, p)

    def finish_end(i):
        j = column(i)
        lanes = pl.ds(pl.multiple_of(j * cw, cw), cw)
        for p, ((lo, n), got) in enumerate(zip(inward(i), fin_copies(i))):
            at = pl.ds(lo, n)
            got.wait_recv()
            out_ref[t, at, lanes] = add(sm[j, 0, at], r_fin[j, at]).astype(jnp.bfloat16)
            share(i, p)

    def forward(i):
        for copies in share_copies(i):
            copies[0].wait_recv()
            copies[2].start()

    @pl.when(is_end)
    def _():
        down_chunk(0)
        pair_sum(0)
        settle(DOWN, 1)
        relay(DOWN, 2)
        spread(DOWN, 3)
        down_chunk(1)
        down_chunk(2)
        pair_sum(1)
        pair_sum(2)
        end_rest(2)
        settle(DOWN, 2)
        down_chunk(3)
        pair_sum(3)
        end_rest(3)
        relay(DOWN, 3)
        settle(DOWN, 3)
        down_chunk(4)
        down_chunk(5)
        pair_sum(4)
        pair_sum(5)

    @pl.when(is_mid)
    def _():
        settle(DOWN, 1)
        down_chunk(0)
        down_chunk(1)
        pair_sum(0)
        down_chunk(2)
        pair_sum(1)
        pair_sum(2)
        spread(DOWN, 2)
        spread(DOWN, 3)
        relay(DOWN, 2)
        pass_on(0)
        pass_on(1)
        relay(DOWN, 3)
        settle(DOWN, 2)
        down_chunk(3)
        pair_sum(3)
        pass_on(2)
        settle(DOWN, 3)
        down_chunk(4)
        down_chunk(5)
        pair_sum(4)
        pair_sum(5)

    def weights_sent(a):
        wait_sent(stretch(a, 3), w_send.at[a, 0])
        wait_sent(stretch(a, 8), w_send.at[a, 1])
        wait_sent(stretch(a, 4), w_send.at[a, 2])

    def tokens_sent(mid):
        wait_sent(xn.at[:, 0], td_send)
        for lane in range(len(token_lanes(mid))):
            wait_sent(xn.at[0, 0], t_send.at[lane])

    def pairs_sent():
        wait_sent(pc, c_send)

    @pl.when(is_mid)
    def _():
        hand_back(5)
        hand_back(4)
        pass_on(3)
        hand_back(3)
        finish_mid(3)
        weights_sent(GATE)
        pass_on(4)
        hand_back(2)
        finish_mid(2)
        pass_on(5)
        forward(3)
        hand_back(1)
        finish_mid(4)
        finish_mid(5)
        hand_back(0)
        forward(2)
        finish_mid(1)
        finish_mid(0)
        weights_sent(UP)
        weights_sent(DOWN)
        forward(4)
        tokens_sent(True)
        forward(5)
        pairs_sent()
        forward(1)
        forward(0)

    @pl.when(is_end)
    def _():
        end_rest(4, 5, 1, 0)
        finish_end(5)
        finish_end(4)
        weights_sent(GATE)
        forward(5)
        finish_end(3)
        forward(4)
        weights_sent(UP)
        weights_sent(DOWN)
        finish_end(2)
        forward(3)
        tokens_sent(False)
        finish_end(1)
        forward(2)
        pairs_sent()
        finish_end(0)
        forward(1)
        forward(0)

    def complete_piece(tt):
        v = out_ref[tt].astype(jnp.float32)
        scale = lax.rsqrt(jnp.mean(v * v, axis=-1, keepdims=True) + epsilon)
        xs[tt] = (xs[tt].astype(jnp.float32) + v * scale * gains[1]).astype(jnp.bfloat16)
        pltpu.make_async_copy(xs.at[tt], result_ref.at[tt], w_sem).start()

    complete_piece(t)
    complete_piece((t + 2) % 4)
    for n in range(2):
        wait_got(out_ref.at[0], oc_recv.at[n])
        complete_piece((t + 1 - 2 * c + 2 * n) % 4)
    wait_sent(out_ref.at[pl.ds(0, 3)], o_send)

    @pl.when(is_end)
    def _():
        wait_sent(r_end, e_send)

    @pl.when(is_mid)
    def _():
        wait_sent(r_mid, m_send)
        wait_sent(r_fin, f_send)

    pltpu.make_async_copy(xs, result_ref, w_sem).wait()


def fused(tokens, norm_gain, gate_weight, up_weight, down_weight, branch_gain):
    rows, d = tokens.shape
    n_tp, planes = 4, 4
    rq = rows // n_tp
    hidden = gate_weight.shape[1]
    width = 2 * (hidden // planes)
    chunks = 2 * SUB
    cw = d // chunks
    bf16, f32, dma = jnp.bfloat16, jnp.float32, pltpu.SemaphoreType.DMA
    hbm = pl.BlockSpec(memory_space=pl.ANY)
    out = pl.pallas_call(
        kernel,
        out_shape=jax.ShapeDtypeStruct((n_tp, rq, d), bf16),
        in_specs=[hbm] * 6,
        out_specs=hbm,
        scratch_shapes=[
            pltpu.VMEM((n_tp, rq, d), bf16),
            pltpu.VMEM((2, 1, d), f32),
            pltpu.VMEM((n_tp, rq, d), bf16),
            pltpu.VMEM((planes, 2, rq, d), bf16),
            pltpu.VMEM((d, width), bf16),
            pltpu.VMEM((d, width), bf16),
            pltpu.VMEM((d, width), bf16),
            pltpu.VMEM((planes, 2 * rq, width), f32),
            pltpu.VMEM((planes, 2 * rq, width), bf16),
            pltpu.VMEM((chunks, planes, 2, rq, cw), bf16),
            pltpu.VMEM((chunks, planes, rq, cw), bf16),
            pltpu.VMEM((chunks, planes, rq, cw), bf16),
            pltpu.VMEM((chunks, 3, rq, cw), bf16),
            pltpu.VMEM((chunks, 2, rq, cw), bf16),
            pltpu.VMEM((chunks, rq, cw), bf16),
            dma((6,)), dma((7,)), dma((3, 3)), dma((5,)),
            dma((3, 4)), dma((3, 4)), dma((3, 4)),
            dma((3, rq // STRIP)), dma((4,)), dma((chunks,)),
            dma((chunks, 3)), dma((chunks, 2)), dma((chunks, 2)), dma((chunks, 2)), dma((2,)),
        ],
        compiler_params=pltpu.CompilerParams(
            collective_id=0, has_side_effects=True, vmem_limit_bytes=60 * 1024 * 1024
        ),
    )(
        tokens.reshape(n_tp, rq, d), gate_weight, up_weight, down_weight.T, norm_gain, branch_gain,
    )
    return out.reshape(rows, d)


def solution(mesh):
    n_fs, n_tp = mesh.shape["fs"], mesh.shape["tp"]

    def per_device(*args):
        tokens, _, gate_weight = args[:3]
        rows, d = tokens.shape
        depth, hidden = gate_weight.shape
        fits = (
            n_fs == 8
            and n_tp == 4
            and rows % (STRIP * n_tp) == 0
            and depth % (2 * STRIP) == 0
            and hidden % (128 * 4) == 0
            and d % (128 * 2 * SUB) == 0
        )
        if fits:
            return fused(*args)
        return plain(*args)

    in_specs = (P("fs", None), P(), P("fs", "tp"), P("fs", "tp"), P("tp", "fs"), P())
    return jax.shard_map(
        per_device, mesh=mesh, in_specs=in_specs, out_specs=P("fs", None), check_vma=False
    )
```
